32 devices in a mesh: kv: 8 (over z, y), tp: 4 (over x, core).
Axes of the slice: x: 2, y: 2, z: 4, core: 2. Of those that a mesh axis runs over, the one named last changes fastest.
Arguments:
- tokens: bfloat16 [2048, 2048], P('kv'), may hold values from -6 to 6
- query_weight: bfloat16 [2048, 2048], P(None, 'tp'), may hold values from -0.125 to 0.125
- key_weight: bfloat16 [2048, 512], P(None, 'tp'), may hold values from -0.125 to 0.125
- value_weight: bfloat16 [2048, 512], P(None, 'tp'), may hold values from -0.125 to 0.125
- gate_weight: bfloat16 [2048, 64], replicated, may hold values from -0.125 to 0.125
- query_gain: float32 [64], replicated
- key_gain: float32 [64], replicated
- out_weight: bfloat16 [2048, 2048], P('tp'), may hold values from -0.125 to 0.125
- shared_block: int32 [8], P('kv'), may hold values from 0 to 3, as said below
- chosen_device: int32 [32, 7], P('kv'), may hold values from 0 to 7, as said below
Outputs:
- mixed_out: bfloat16 [2048, 2048], P(('kv', 'tp'))
- log_weight: float32 [2, 2048, 32], P(None, 'kv', 'tp')
The draws below stay inside these ranges and needn't reach their ends.
Inputs may be any that keep to these rules, and one draw needn't show every extreme that they name: `shared_block`: entry d names one of the 64-position blocks of device d's 256 positions. `chosen_device`: row b names 7 different devices, never the device that holds query block b.
All inputs are finite; a program needn't handle non-finite values.
Results may differ from the reference program's by a relative error of at most 0.019.
The reference program's roundings to bfloat16 on the way count: a program that leaves them out, or rounds other values in their place, can miss the bound.
Values may be sent and summed in bfloat16 or wider, within the bound.
A program may use at most 64 MiB of HBM per device.

```python
import jax
import jax.numpy as jnp
from jax import lax

D = 2048
H = 32
HD = 64
G = 8
TOK_DEV = 256
SEL = 64
CMP = 32
NREM = 7
SEQ = 2048
NQB = 32
N_KV = 8
N_TP = 4


def plan_blocks(key):
    per_device = TOK_DEV // SEL
    shared_numbers = jax.random.randint(jax.random.fold_in(key, 11), (N_KV,), 0, per_device)
    owning_devices = jnp.arange(N_KV, dtype=jnp.int32)
    home_device = jnp.arange(NQB, dtype=jnp.int32) // per_device
    frequent_blocks = jax.random.randint(jax.random.fold_in(key, 12), (N_KV,), 0, 4) == 0
    added_reward = jnp.where(frequent_blocks, 2048, 0)
    noise_values = jax.random.randint(jax.random.fold_in(key, 13), (NQB, N_KV), 0, 2048)
    forced = (owning_devices[None, :] == home_device[:, None] - 1) | (owning_devices[None, :] == home_device[:, None] - N_KV // 2) & (home_device[:, None] >= N_KV // 2)
    earlier = owning_devices[None, :] < home_device[:, None]
    block_priority = jnp.where(owning_devices[None, :] == home_device[:, None], 0, jnp.where(forced, 3, jnp.where(earlier, 2, 1)))
    block_ranking = (block_priority * 4096 + added_reward[None, :] + noise_values) * N_KV + owning_devices[None, :]
    ignored, selected = lax.top_k(block_ranking, NREM)
    return (shared_numbers.astype(jnp.int32), selected.astype(jnp.int32))


def draw_shared_block(key, part):
    return plan_blocks(key)[0]


def draw_chosen_device(key, part):
    return plan_blocks(key)[1]


def draw_query_gain(key, part):
    return jax.random.uniform(jax.random.fold_in(key, 21), (HD,), jnp.float32, 0.6, 1.6)


def draw_key_gain(key, part):
    return jax.random.uniform(jax.random.fold_in(key, 22), (HD,), jnp.float32, 0.6, 1.6)


def level_of(rng, shape, cuts, least, largest):
    def one(dim, shards_of):
        heights = jax.random.uniform(jax.random.fold_in(jax.random.fold_in(rng, 6), dim), (shards_of,), jnp.float32, least / len(cuts), largest / len(cuts))
        return jnp.repeat(jnp.exp(heights), shape[dim] // shards_of).reshape((-1,) + (1,) * (len(shape) - dim - 1))

    level = one(*cuts[0])
    for cut in cuts[1:]:
        level = level * one(*cut)
    return level


def centred(rng, dims, width, bound, shards=(), kind=jnp.bfloat16):
    array = jax.random.normal(rng, dims, jnp.float32) * width
    if len(shards) > 0:
        array = level_of(rng, dims, shards, -0.22, 0.18) * array
    return jnp.clip(array, min=-bound, max=bound).astype(kind)


def setup_inputs(seed: int = 0) -> dict:
    seeds = jax.random.split(jax.random.key(seed), 11)
    tokens = centred(seeds[0], (SEQ, D), 1.0, 6.0, ((0, 8),))
    query_weight = centred(seeds[1], (D, H * HD), D ** -0.5, 0.125, ((1, 4),))
    key_weight = centred(seeds[2], (D, G * HD), D ** -0.5, 0.125, ((1, 4),))
    value_weight = centred(seeds[3], (D, G * HD), D ** -0.5, 0.125, ((1, 4),))
    gate_weight = centred(seeds[4], (D, 2 * H), D ** -0.5, 0.125)
    query_gain = draw_query_gain(jax.random.fold_in(seeds[10], 71), 0)
    key_gain = draw_key_gain(jax.random.fold_in(seeds[10], 71), 0)
    out_weight = centred(seeds[7], (H * HD, D), (H * HD) ** -0.5, 0.125, ((0, 4),))
    shared_block = draw_shared_block(jax.random.fold_in(seeds[10], 71), 0)
    chosen_device = draw_chosen_device(jax.random.fold_in(seeds[10], 71), 0)
    return {"tokens": tokens, "query_weight": query_weight, "key_weight": key_weight, "value_weight": value_weight, "gate_weight": gate_weight, "query_gain": query_gain, "key_gain": key_gain, "out_weight": out_weight, "shared_block": shared_block, "chosen_device": chosen_device}


norm_eps = 1e-06
rope_base = 500000.0
big_negative = -1e+30

def rounded(values_in):
    return lax.optimization_barrier(values_in.astype(jnp.bfloat16))

def unit_norm(values_in, gain_vec):
    upcast = values_in.astype(jnp.float32)
    return upcast * lax.rsqrt(lax.optimization_barrier(jnp.mean(upcast * upcast, axis=-1, keepdims=True)) + norm_eps) * gain_vec

def rotate(values_in, places):
    half_size = values_in.shape[-1] // 2
    inverse = jnp.power(rope_base, -jnp.arange(half_size, dtype=jnp.float32) * 2.0 / values_in.shape[-1])
    angles = places.astype(jnp.float32)[:, None] * inverse[None, :]
    cos_vals = jnp.cos(angles)[:, None, :]
    sin_vals = jnp.sin(angles)[:, None, :]
    upcast = values_in.astype(jnp.float32)
    front_half = upcast[..., :half_size]
    back_half = upcast[..., half_size:]
    return jnp.concatenate([front_half * cos_vals - back_half * sin_vals, back_half * cos_vals + front_half * sin_vals], axis=-1)

def reference(tokens, query_weight, key_weight, value_weight, gate_weight, query_gain, key_gain, out_weight, shared_block, chosen_device):
    seq_len = tokens.shape[0]
    per_group = H // G
    places = jnp.arange(seq_len, dtype=jnp.int32)
    queries = rounded(jnp.dot(tokens, query_weight, preferred_element_type=jnp.float32)).reshape(seq_len, H, HD)
    keys_raw = rounded(jnp.dot(tokens, key_weight, preferred_element_type=jnp.float32)).reshape(seq_len, G, HD)
    values_raw = rounded(jnp.dot(tokens, value_weight, preferred_element_type=jnp.float32)).reshape(seq_len, G, HD)
    q_plain = rounded(unit_norm(queries, query_gain))
    k_plain = rounded(unit_norm(keys_raw, key_gain))
    q_turned = rounded(rotate(q_plain, places))
    k_turned = rounded(rotate(k_plain, places))
    gate_vals = jax.nn.sigmoid(jnp.dot(tokens, gate_weight, preferred_element_type=jnp.float32)).reshape(seq_len, H, 2)
    span_count = seq_len // CMP
    span_keys = rounded(lax.optimization_barrier(jnp.mean(k_plain.astype(jnp.float32).reshape(span_count, CMP, G, HD), axis=1))).astype(jnp.float32)
    span_values = rounded(lax.optimization_barrier(jnp.mean(values_raw.astype(jnp.float32).reshape(span_count, CMP, G, HD), axis=1))).astype(jnp.float32)
    span_ends = jnp.arange(span_count, dtype=jnp.int32) * CMP + CMP - 1
    blocks_dev = TOK_DEV // SEL
    block_numbers = (chosen_device * blocks_dev + shared_block[chosen_device]).astype(jnp.int32)
    key_blocks = k_turned.reshape(NQB, SEL, G, HD)
    value_blocks = values_raw.reshape(NQB, SEL, G, HD)
    score_scale = HD ** (-0.5)
    causal_own = jnp.arange(SEL)[None, :] <= jnp.arange(SEL)[:, None]

    def one_block(inputs):
        q_plain_b, q_turned_b, named_blocks, devices_named, block_num = inputs
        qplaces = block_num * SEL + jnp.arange(SEL, dtype=jnp.int32)
        scores = jnp.einsum('qghd,cgd->qghc', q_plain_b.astype(jnp.float32), span_keys) * score_scale
        allowed = (span_ends[None, :] <= qplaces[:, None])[:, None, None, :]
        has_span = (qplaces >= CMP - 1)[:, None, None]
        peak_val = lax.optimization_barrier(jnp.max(jnp.where(allowed, scores, big_negative), axis=-1))
        weights_raw = jnp.where(allowed, jnp.exp(scores - peak_val[..., None]), 0.0)
        divisor = jnp.where(has_span, lax.optimization_barrier(jnp.sum(weights_raw, axis=-1)), 1.0)
        span_out = jnp.einsum('qghc,cgd->qghd', rounded(weights_raw).astype(jnp.float32), span_values) / divisor[..., None]
        span_lse = jnp.where(has_span, peak_val + jnp.log(divisor), 0.0)
        key_rows = jnp.concatenate([key_blocks[block_num][None], key_blocks[named_blocks]], axis=0).reshape(-1, G, HD).astype(jnp.float32)
        value_rows = jnp.concatenate([value_blocks[block_num][None], value_blocks[named_blocks]], axis=0).reshape(-1, G, HD).astype(jnp.float32)
        remote_ok = jnp.repeat(devices_named < block_num // blocks_dev, SEL)
        allowed_sel = jnp.concatenate([causal_own, jnp.broadcast_to(remote_ok[None, :], (SEL, remote_ok.shape[0]))], axis=1)[:, None, None, :]
        scores_sel = jnp.einsum('qghd,kgd->qghk', q_turned_b.astype(jnp.float32), key_rows) * score_scale
        peak_sel = lax.optimization_barrier(jnp.max(jnp.where(allowed_sel, scores_sel, big_negative), axis=-1))
        weights_sel = jnp.where(allowed_sel, jnp.exp(scores_sel - peak_sel[..., None]), 0.0)
        sum_sel = lax.optimization_barrier(jnp.sum(weights_sel, axis=-1))
        chosen_out = jnp.einsum('qghk,kgd->qghd', rounded(weights_sel).astype(jnp.float32), value_rows) / sum_sel[..., None]
        return (span_out, chosen_out, span_lse, peak_sel + jnp.log(sum_sel))
    span_out, chosen_out, span_lse, chosen_lse = lax.map(one_block, (q_plain.reshape(NQB, SEL, G, per_group, HD), q_turned.reshape(NQB, SEL, G, per_group, HD), block_numbers, chosen_device, jnp.arange(NQB, dtype=jnp.int32)))
    span_out = span_out.reshape(seq_len, H, HD)
    chosen_out = chosen_out.reshape(seq_len, H, HD)
    mixed_heads = rounded(gate_vals[..., 0:1] * span_out + gate_vals[..., 1:2] * chosen_out).reshape(seq_len, H * HD)
    group_width = H * HD // N_TP
    accum_sum = jnp.zeros((seq_len, D), jnp.float32)
    for group_num in range(N_TP):
        partial_value = jnp.dot(mixed_heads[:, group_num * group_width:(group_num + 1) * group_width], out_weight[group_num * group_width:(group_num + 1) * group_width], preferred_element_type=jnp.float32)
        accum_sum = accum_sum + rounded(partial_value).astype(jnp.float32)
    mixed_out = accum_sum.astype(jnp.bfloat16)
    log_weight = jnp.stack([span_lse.reshape(seq_len, H), chosen_lse.reshape(seq_len, H)])
    return (mixed_out, log_weight)
```

```python
import functools

import jax
import jax.numpy as jnp
import numpy as np
from jax import lax
from jax.experimental import pallas as pl
from jax.experimental.pallas import tpu as pltpu
from jax.sharding import PartitionSpec as P

SEL = 64
CMP = 32
LANES = 128
SPAN_PAD = 16

norm_eps = 1e-06
rope_base = 500000.0
big_negative = -1e30

F32 = jnp.float32
BF16 = jnp.bfloat16
MESH = pl.DeviceIdType.MESH


def mm(a, b):
    return lax.dot_general(a, b, (((1,), (0,)), ((), ())), preferred_element_type=F32)


def mm_t(a, b):
    return lax.dot_general(a, b, (((1,), (1,)), ((), ())), preferred_element_type=F32)


def iota(shape, dim):
    return lax.broadcasted_iota(jnp.int32, shape, dim)


def tile_lanes(row, times):
    return row if times == 1 else jnp.concatenate([row] * times, axis=1)


def layer_kernel(
    n_kv, n_tp, heads, groups, head_size,
    tok_hbm, wq_hbm, wk_hbm, wv_hbm, wg_hbm, wo_hbm, tab_hbm, base_hbm,
    qgain_ref, kgain_ref, shared_ref, chosen_ref,
    out_ref, lse_ref,
    tok, wq, wkv, wg, wo, tab, base,
    own, slab, gath, qp_heads, qt_heads, gates, mixed, lse_rows,
    pair_send, pair_recv, cross_send, cross_recv,
    load_sem, slab_ss, slab_rs, pair_ss, pair_rs, cross_ss, cross_rs,
):
    rows = tok.shape[0]
    per_group = heads // groups
    half = LANES // 2
    n_x = n_tp // 2
    chunk = rows // n_tp
    n_chosen = chosen_ref.shape[1]
    me = lax.axis_index("kv")
    my_tp = lax.axis_index("tp")
    my_x = my_tp // 2
    my_core = my_tp % 2

    loads = [
        pltpu.make_async_copy(src, dst, load_sem.at[i])
        for i, (src, dst) in enumerate([
            (tok_hbm, tok),
            (wk_hbm, wkv.at[:, 0:LANES]),
            (wv_hbm, wkv.at[:, LANES:2 * LANES]),
            (tab_hbm, tab),
            (base_hbm, base),
            (wq_hbm, wq),
            (wg_hbm, wg),
            (wo_hbm, wo),
        ])
    ]
    for copy in loads:
        copy.start()

    barrier = pltpu.get_barrier_semaphore()

    def greet_kv(d, carry):
        @pl.when(d != me)
        def _():
            pl.semaphore_signal(barrier, inc=1, device_id={"kv": d}, device_id_type=MESH)
        return carry

    lax.fori_loop(0, n_kv, greet_kv, 0)
    for t in range(1, n_tp):
        peer = lax.rem(my_tp + t, n_tp)
        pl.semaphore_signal(barrier, inc=1, device_id={"tp": peer}, device_id_type=MESH)

    def clear(d, carry):
        gath[d] = jnp.zeros(gath.shape[1:], BF16)
        return carry

    lax.fori_loop(me + 1, n_kv, clear, 0)

    big = 2 * LANES
    row_i = iota((big, big), 0)
    col_i = iota((big, big), 1)
    block_mean = jnp.where(row_i // head_size == col_i // head_size, 1.0 / head_size, 0.0).astype(BF16)
    hs2 = head_size // 2
    first = (col_i % head_size) < hs2
    swap = jnp.where(
        first & (row_i == col_i + hs2), -1.0,
        jnp.where((~first) & (row_i == col_i - hs2), 1.0, 0.0),
    ).astype(BF16)

    def by_tiles(x, mat):
        width = x.shape[1]
        step = min(width, big)
        parts = [mm(x[:, i:i + step], mat[:step, :step]) for i in range(0, width, step)]
        return parts[0] if len(parts) == 1 else jnp.concatenate(parts, axis=1)

    def unit_norm(x, gain_row):
        sq = x * x
        hi = sq.astype(BF16)
        lo = (sq - hi.astype(F32)).astype(BF16)
        mean = by_tiles(hi, block_mean) + by_tiles(lo, block_mean)
        return (x * lax.rsqrt(mean + norm_eps) * gain_row).astype(BF16)

    loads[3].wait()
    loads[4].wait()
    cos_b = base[0, pl.ds(me, 1), :]
    sin_b = base[1, pl.ds(me, 1), :]
    cos_t = tab[0] * cos_b - tab[1] * sin_b
    sin_t = tab[1] * cos_b + tab[0] * sin_b

    def rotate(x):
        times = x.shape[1] // LANES
        return x.astype(F32) * tile_lanes(cos_t, times) + by_tiles(x, swap) * tile_lanes(sin_t, times)

    loads[0].wait()
    loads[1].wait()
    loads[2].wait()
    tokens = tok[...]
    kv_raw = mm(tokens, wkv[...]).astype(BF16)
    values = kv_raw[:, LANES:]
    k_gain = tile_lanes(kgain_ref[...], LANES // head_size)
    k_plain = unit_norm(kv_raw[:, :LANES].astype(F32), k_gain)
    k_turned = rotate(k_plain).astype(BF16)
    own[:, :LANES] = k_turned
    own[:, LANES:] = values
    spans_dev = rows // CMP
    avg = jnp.where(
        iota((SPAN_PAD, rows), 1) // CMP == iota((SPAN_PAD, rows), 0), 1.0 / CMP, 0.0
    ).astype(BF16)
    summary_k = mm(avg, k_plain).astype(BF16)
    summary_v = mm(avg, values).astype(BF16)
    slab[SEL:, :LANES] = summary_k
    slab[SEL:, LANES:] = summary_v
    gath[me, SEL:, :LANES] = summary_k
    gath[me, SEL:, LANES:] = summary_v
    pick = iota((SEL, rows), 1) == iota((SEL, rows), 0) + shared_ref[0] * SEL
    pick = jnp.where(pick, 1.0, 0.0).astype(BF16)
    slab[:SEL, :LANES] = mm(pick, k_turned).astype(BF16)
    slab[:SEL, LANES:] = mm(pick, values).astype(BF16)

    pl.semaphore_wait(barrier, n_kv - 1 + n_tp - 1)

    def slab_copy(slot, dst):
        return pltpu.make_async_remote_copy(
            src_ref=slab, dst_ref=gath.at[slot],
            send_sem=slab_ss.at[dst], recv_sem=slab_rs.at[slot],
            device_id={"kv": dst}, device_id_type=MESH,
        )

    def send_slab(i, carry):
        slab_copy(me, n_kv - 1 - i).start()
        return carry

    lax.fori_loop(0, n_kv - 1 - me, send_slab, 0)

    loads[5].wait()
    lane = iota((rows, LANES), 1)
    q_raw = mm(tokens, wq[...]).astype(BF16).astype(F32)
    q_gain = tile_lanes(qgain_ref[...], heads)
    q_plain = unit_norm(q_raw, q_gain)
    q_turned = rotate(q_plain).astype(BF16).astype(F32)
    q_plain = q_plain.astype(F32)
    scale = head_size ** (-0.5)
    for source, target in ((q_plain, qp_heads), (q_turned, qt_heads)):
        for h in range(heads):
            group = h // per_group
            part = source[:, (h // 2) * LANES:(h // 2 + 1) * LANES] * scale
            if h % 2 != group % 2:
                part = pltpu.roll(part, half, 1)
            target[h] = jnp.where((lane // half) == group % 2, part, 0.0).astype(BF16)
    loads[6].wait()
    gate_all = jax.nn.sigmoid(mm_t(tokens, wg[...]))
    gate_cols = gate_all.shape[1]
    gate_pad = jnp.concatenate([gate_all, jnp.zeros((rows, LANES - gate_cols), F32)], axis=1)
    gates[...] = pltpu.roll(gate_pad, lax.rem(LANES - my_tp * 2 * heads, LANES), 1)

    def wait_slab(d, carry):
        slab_copy(d, me).wait_recv()
        return carry

    lax.fori_loop(0, me, wait_slab, 0)
    loads[7].wait()

    slab_devs = min(n_kv, 8)
    n_slabs = n_kv // slab_devs
    stacked = heads * chunk
    sel_lane = iota((chunk, slab_devs * SEL), 1)
    sel_row = iota((chunk, slab_devs * SEL), 0)
    span_lane = iota((chunk, n_kv * SPAN_PAD), 1)
    span_row = iota((chunk, n_kv * SPAN_PAD), 0)
    span_keys = gath[:, SEL:, :LANES].reshape(n_kv * SPAN_PAD, LANES)
    span_values = gath[:, SEL:, LANES:].reshape(n_kv * SPAN_PAD, LANES)
    span_id = (span_lane // SPAN_PAD) * spans_dev + span_lane % SPAN_PAD
    chunk_lane = iota((chunk, LANES), 1)

    def masked(scores, mask):
        cube = scores.reshape(heads, chunk, scores.shape[1])
        return jnp.where(mask[None], cube, big_negative).reshape(scores.shape)

    def attend(which, slot_rows):
        start = pl.multiple_of(which * chunk, chunk)
        local_block = start // SEL
        block_start = pl.multiple_of(local_block * SEL, SEL)
        in_block = start - block_start
        gath[me, :SEL, :] = own[pl.ds(block_start, SEL), :]

        qp = qp_heads[:, pl.ds(start, chunk), :].reshape(stacked, LANES)
        qt = qt_heads[:, pl.ds(start, chunk), :].reshape(stacked, LANES)

        place = me * rows + start + span_row
        allowed = (span_lane % SPAN_PAD < spans_dev) & (span_id * CMP + CMP - 1 <= place)
        s = masked(mm_t(qp, span_keys), allowed)
        span_peak = jnp.max(s, axis=1, keepdims=True)
        w = jnp.exp(s - span_peak)
        span_sum = jnp.sum(w, axis=1, keepdims=True)
        span_out = mm(w.astype(BF16), span_values)

        def slab_step(i, carry):
            base_dev = i * slab_devs
            keys = gath[pl.ds(base_dev, slab_devs), :SEL, :LANES].reshape(slab_devs * SEL, LANES)
            vals = gath[pl.ds(base_dev, slab_devs), :SEL, LANES:].reshape(slab_devs * SEL, LANES)
            dev = base_dev + sel_lane // SEL
            member = dev == chosen_ref[local_block, 0]
            for j in range(1, n_chosen):
                member = member | (dev == chosen_ref[local_block, j])
            ok = (member & (dev < me)) | ((dev == me) & (sel_lane % SEL <= sel_row + in_block))
            sc = masked(mm_t(qt, keys), ok)
            peak = jnp.max(sc, axis=1, keepdims=True)
            if carry is None:
                e = jnp.exp(sc - peak)
                return peak, jnp.sum(e, axis=1, keepdims=True), mm(e.astype(BF16), vals)
            old_peak, old_sum, old_out = carry
            peak = jnp.maximum(peak, old_peak)
            factor = jnp.exp(old_peak - peak)
            e = jnp.exp(sc - peak) * jnp.where(sc > 0.5 * big_negative, 1.0, 0.0)
            return (
                peak,
                old_sum * factor + jnp.sum(e, axis=1, keepdims=True),
                old_out * factor + mm(e.astype(BF16), vals),
            )

        if n_slabs == 1:
            sel_peak, sel_sum, sel_out = slab_step(0, None)
        else:
            sel_peak, sel_sum, sel_out = lax.fori_loop(
                0, n_slabs, slab_step,
                (
                    jnp.full((stacked, 1), big_negative, F32),
                    jnp.zeros((stacked, 1), F32),
                    jnp.zeros((stacked, LANES), F32),
                ),
            )

        has_span = (me * rows + start + iota((chunk, 1), 0)) >= CMP - 1
        gate = gates[pl.ds(start, chunk), :]
        lse0 = jnp.zeros((chunk, LANES), F32)
        lse1 = jnp.zeros((chunk, LANES), F32)
        even = None
        for h in range(heads):
            piece = slice(h * chunk, (h + 1) * chunk)
            ssum = jnp.where(has_span, span_sum[piece], 1.0)
            g0 = jnp.where(has_span, gate[:, 2 * h:2 * h + 1] / ssum, 0.0)
            g1 = gate[:, 2 * h + 1:2 * h + 2] / sel_sum[piece]
            l0 = jnp.where(has_span, span_peak[piece] + jnp.log(ssum), 0.0)
            l1 = sel_peak[piece] + jnp.log(sel_sum[piece])
            lse0 = jnp.where(chunk_lane == h, l0, lse0)
            lse1 = jnp.where(chunk_lane == h, l1, lse1)
            both = g0 * span_out[piece] + g1 * sel_out[piece]
            if h % 2 != (h // per_group) % 2:
                both = pltpu.roll(both, half, 1)
            if h % 2 == 0:
                even = both
            else:
                pair = jnp.where(chunk_lane < half, even, both).astype(BF16)
                mixed[slot_rows:slot_rows + chunk, (h // 2) * LANES:(h // 2 + 1) * LANES] = pair
        lse_rows[0, pl.ds(start, chunk), :] = lse0
        lse_rows[1, pl.ds(start, chunk), :] = lse1

    def pair_copy(t):
        return pltpu.make_async_remote_copy(
            src_ref=pair_send.at[t], dst_ref=pair_recv.at[t],
            send_sem=pair_ss.at[t], recv_sem=pair_rs.at[t],
            device_id={"tp": my_x * 2 + 1 - my_core}, device_id_type=MESH,
        )

    def cross_copy(t):
        return pltpu.make_async_remote_copy(
            src_ref=cross_send.at[t - 1], dst_ref=cross_recv.at[t - 1],
            send_sem=cross_ss.at[t - 1], recv_sem=cross_rs.at[t - 1],
            device_id={"tp": lax.rem(my_x + t, n_x) * 2 + my_core}, device_id_type=MESH,
        )

    for t in range(n_x - 1, -1, -1):
        chip = lax.rem(my_x + t, n_x)
        attend(chip * 2 + 1 - my_core, 0)
        attend(chip * 2 + my_core, chunk)
        partial = mm(mixed[...], wo[...])
        pair_send[t] = partial[:chunk].astype(BF16)
        pair_copy(t).start()
        mine = partial[chunk:]
        pair_copy(t).wait_recv()
        mine = mine + pair_recv[t].astype(F32)
        if t > 0:
            cross_send[t - 1] = mine.astype(BF16)
            cross_copy(t).start()
        else:
            for u in range(n_x - 1, 0, -1):
                cross_copy(u).wait_recv()
                mine = mine + cross_recv[u - 1].astype(F32)
            out_ref[...] = mine.astype(BF16)
            for b in range(2):
                lse_ref[b] = jnp.transpose(lse_rows[b])[:heads]

    for t in range(n_x):
        pair_copy(t).wait_send()
        if t > 0:
            cross_copy(t).wait_send()

    def wait_sent(i, carry):
        slab_copy(me, n_kv - 1 - i).wait_send()
        return carry

    lax.fori_loop(0, n_kv - 1 - me, wait_sent, 0)


def rope_tables(rows, n_kv, head_size):
    inverse = np.power(rope_base, -np.arange(head_size // 2, dtype=np.float64) * 2.0 / head_size)
    inverse = np.tile(inverse, LANES // (head_size // 2))[None, :]
    near = np.arange(rows, dtype=np.float64)[:, None] * inverse
    far = np.arange(n_kv, dtype=np.float64)[:, None] * rows * inverse
    stack = lambda a: np.stack([np.cos(a), np.sin(a)]).astype(np.float32)
    return stack(near), stack(far)


def shards(
    n_kv, n_tp,
    tokens, query_weight, key_weight, value_weight, gate_weight,
    query_gain, key_gain, out_weight, shared_block, chosen_device,
):
    rows, width = tokens.shape
    head_size = query_gain.shape[0]
    heads = query_weight.shape[1] // head_size
    group_width = key_weight.shape[1]
    groups = group_width // head_size
    if group_width < LANES:
        pad = ((0, 0), (0, LANES - group_width))
        key_weight = jnp.pad(key_weight, pad)
        value_weight = jnp.pad(value_weight, pad)
    n_x = n_tp // 2
    chunk = rows // n_tp
    inner = heads * head_size
    d_out = out_weight.shape[1]
    near, far = rope_tables(rows, n_kv, head_size)
    hbm = pl.BlockSpec(memory_space=pl.ANY)
    vmem = pl.BlockSpec(memory_space=pltpu.VMEM)
    smem = pl.BlockSpec(memory_space=pltpu.SMEM)
    dma = pltpu.SemaphoreType.DMA
    mixed_out, lse = pl.pallas_call(
        functools.partial(layer_kernel, n_kv, n_tp, heads, groups, head_size),
        out_shape=(
            jax.ShapeDtypeStruct((chunk, d_out), BF16),
            jax.ShapeDtypeStruct((2, heads, rows), F32),
        ),
        in_specs=[hbm] * 8 + [vmem] * 2 + [smem] * 2,
        out_specs=(vmem, vmem),
        scratch_shapes=[
            pltpu.VMEM((rows, width), BF16),
            pltpu.VMEM((width, inner), BF16),
            pltpu.VMEM((width, 2 * LANES), BF16),
            pltpu.VMEM(gate_weight.shape[::-1], BF16),
            pltpu.VMEM((inner, d_out), BF16),
            pltpu.VMEM(near.shape, F32),
            pltpu.VMEM(far.shape, F32),
            pltpu.VMEM((rows, 2 * LANES), BF16),
            pltpu.VMEM((SEL + SPAN_PAD, 2 * LANES), BF16),
            pltpu.VMEM((n_kv, SEL + SPAN_PAD, 2 * LANES), BF16),
            pltpu.VMEM((heads, rows, LANES), BF16),
            pltpu.VMEM((heads, rows, LANES), BF16),
            pltpu.VMEM((rows, LANES), F32),
            pltpu.VMEM((2 * chunk, inner), BF16),
            pltpu.VMEM((2, rows, LANES), F32),
            pltpu.VMEM((n_x, chunk, d_out), BF16),
            pltpu.VMEM((n_x, chunk, d_out), BF16),
            pltpu.VMEM((n_x - 1, chunk, d_out), BF16),
            pltpu.VMEM((n_x - 1, chunk, d_out), BF16),
            dma((8,)),
            dma((n_kv,)),
            dma((n_kv,)),
            dma((n_x,)),
            dma((n_x,)),
            dma((n_x - 1,)),
            dma((n_x - 1,)),
        ],
        compiler_params=pltpu.CompilerParams(
            collective_id=0, has_side_effects=True, vmem_limit_bytes=60 * 1024 * 1024
        ),
        name="layer",
    )(
        tokens, query_weight, key_weight, value_weight, gate_weight.T, out_weight,
        jnp.asarray(near), jnp.asarray(far),
        query_gain.reshape(1, head_size), key_gain.reshape(1, head_size),
        shared_block, chosen_device,
    )
    return mixed_out, jnp.transpose(lse, (0, 2, 1))


def solution(mesh):
    placed = (
        P("kv", None),
        P(None, "tp"),
        P(None, "tp"),
        P(None, "tp"),
        P(),
        P(),
        P(),
        P("tp", None),
        P("kv"),
        P("kv", None),
    )
    return jax.shard_map(
        functools.partial(shards, mesh.shape["kv"], mesh.shape["tp"]),
        mesh=mesh,
        in_specs=placed,
        out_specs=(P(("kv", "tp"), None), P(None, "kv", "tp")),
        check_vma=False,
    )
```

```python
import functools

import jax
import jax.numpy as jnp
import numpy as np
from jax import lax
from jax.experimental import pallas as pl
from jax.experimental.pallas import tpu as pltpu
from jax.sharding import PartitionSpec as P

SEL = 64
CMP = 32
LANES = 128
SPAN_PAD = 16

norm_eps = 1e-06
rope_base = 500000.0
big_negative = -1e30

F32 = jnp.float32
BF16 = jnp.bfloat16
MESH = pl.DeviceIdType.MESH


def mm(a, b):
    return lax.dot_general(a, b, (((1,), (0,)), ((), ())), preferred_element_type=F32)


def mm_t(a, b):
    return lax.dot_general(a, b, (((1,), (1,)), ((), ())), preferred_element_type=F32)


def iota(shape, dim):
    return lax.broadcasted_iota(jnp.int32, shape, dim)


def tile_lanes(row, times):
    return row if times == 1 else jnp.concatenate([row] * times, axis=1)


def layer_kernel(
    n_kv, n_tp, heads, groups, head_size,
    tok_hbm, wq_hbm, wk_hbm, wv_hbm, wg_hbm, wo_hbm, tab_hbm, base_hbm,
    qgain_ref, kgain_ref, shared_ref, chosen_ref,
    out_ref, lse_ref,
    tok, wq, wkv, wg, wo, tab, base,
    own, slab, gath, qp_heads, qt_heads, gates, mixed, lse_rows,
    pair_send, pair_recv, cross_send, cross_recv,
    load_sem, slab_ss, slab_rs, pair_ss, pair_rs, cross_ss, cross_rs,
):
    rows = tok.shape[0]
    per_group = heads // groups
    half = LANES // 2
    n_x = n_tp // 2
    chunk = rows // n_tp
    n_chosen = chosen_ref.shape[1]
    me = lax.axis_index("kv")
    my_tp = lax.axis_index("tp")
    my_x = my_tp // 2
    my_core = my_tp % 2

    loads = [
        pltpu.make_async_copy(src, dst, load_sem.at[i])
        for i, (src, dst) in enumerate([
            (tok_hbm, tok),
            (wk_hbm, wkv.at[:, 0:LANES]),
            (wv_hbm, wkv.at[:, LANES:2 * LANES]),
            (tab_hbm, tab),
            (base_hbm, base),
            (wq_hbm, wq),
            (wg_hbm, wg),
            (wo_hbm, wo),
        ])
    ]
    for copy in loads:
        copy.start()

    barrier = pltpu.get_barrier_semaphore()

    def greet_kv(d, carry):
        @pl.when(d != me)
        def _():
            pl.semaphore_signal(barrier, inc=1, device_id={"kv": d}, device_id_type=MESH)
        return carry

    lax.fori_loop(0, n_kv, greet_kv, 0)
    for t in range(1, n_tp):
        peer = lax.rem(my_tp + t, n_tp)
        pl.semaphore_signal(barrier, inc=1, device_id={"tp": peer}, device_id_type=MESH)

    def clear(d, carry):
        gath[d] = jnp.zeros(gath.shape[1:], BF16)
        return carry

    lax.fori_loop(me + 1, n_kv, clear, 0)

    big = 2 * LANES
    row_i = iota((big, big), 0)
    col_i = iota((big, big), 1)
    block_mean = jnp.where(row_i // head_size == col_i // head_size, 1.0 / head_size, 0.0).astype(BF16)
    hs2 = head_size // 2
    first = (col_i % head_size) < hs2
    swap = jnp.where(
        first & (row_i == col_i + hs2), -1.0,
        jnp.where((~first) & (row_i == col_i - hs2), 1.0, 0.0),
    ).astype(BF16)

    def by_tiles(x, mat):
        width = x.shape[1]
        step = min(width, big)
        parts = [mm(x[:, i:i + step], mat[:step, :step]) for i in range(0, width, step)]
        return parts[0] if len(parts) == 1 else jnp.concatenate(parts, axis=1)

    def unit_norm(x, gain_row):
        sq = x * x
        hi = sq.astype(BF16)
        lo = (sq - hi.astype(F32)).astype(BF16)
        mean = by_tiles(hi, block_mean) + by_tiles(lo, block_mean)
        return (x * lax.rsqrt(mean + norm_eps) * gain_row).astype(BF16)

    loads[3].wait()
    loads[4].wait()
    cos_b = base[0, pl.ds(me, 1), :]
    sin_b = base[1, pl.ds(me, 1), :]
    cos_t = tab[0] * cos_b - tab[1] * sin_b
    sin_t = tab[1] * cos_b + tab[0] * sin_b

    def rotate(x):
        times = x.shape[1] // LANES
        return x.astype(F32) * tile_lanes(cos_t, times) + by_tiles(x, swap) * tile_lanes(sin_t, times)

    loads[0].wait()
    loads[1].wait()
    loads[2].wait()
    tokens = tok[...]
    kv_raw = mm(tokens, wkv[...]).astype(BF16)
    values = kv_raw[:, LANES:]
    k_gain = tile_lanes(kgain_ref[...], LANES // head_size)
    k_plain = unit_norm(kv_raw[:, :LANES].astype(F32), k_gain)
    k_turned = rotate(k_plain).astype(BF16)
    own[:, :LANES] = k_turned
    own[:, LANES:] = values
    spans_dev = rows // CMP
    avg = jnp.where(
        iota((SPAN_PAD, rows), 1) // CMP == iota((SPAN_PAD, rows), 0), 1.0 / CMP, 0.0
    ).astype(BF16)
    summary_k = mm(avg, k_plain).astype(BF16)
    summary_v = mm(avg, values).astype(BF16)
    slab[SEL:, :LANES] = summary_k
    slab[SEL:, LANES:] = summary_v
    gath[me, SEL:, :LANES] = summary_k
    gath[me, SEL:, LANES:] = summary_v
    pick = iota((SEL, rows), 1) == iota((SEL, rows), 0) + shared_ref[0] * SEL
    pick = jnp.where(pick, 1.0, 0.0).astype(BF16)
    slab[:SEL, :LANES] = mm(pick, k_turned).astype(BF16)
    slab[:SEL, LANES:] = mm(pick, values).astype(BF16)

    pl.semaphore_wait(barrier, n_kv - 1 + n_tp - 1)

    def slab_copy(slot, dst):
        return pltpu.make_async_remote_copy(
            src_ref=slab, dst_ref=gath.at[slot],
            send_sem=slab_ss.at[dst], recv_sem=slab_rs.at[slot],
            device_id={"kv": dst}, device_id_type=MESH,
        )

    def send_slab(i, carry):
        slab_copy(me, n_kv - 1 - i).start()
        return carry

    lax.fori_loop(0, n_kv - 1 - me, send_slab, 0)

    loads[5].wait()
    lane = iota((rows, LANES), 1)
    q_raw = mm(tokens, wq[...]).astype(BF16).astype(F32)
    q_gain = tile_lanes(qgain_ref[...], heads)
    q_plain = unit_norm(q_raw, q_gain)
    q_turned = rotate(q_plain).astype(BF16).astype(F32)
    q_plain = q_plain.astype(F32)
    scale = head_size ** (-0.5)
    for source, target in ((q_plain, qp_heads), (q_turned, qt_heads)):
        for h in range(heads):
            group = h // per_group
            part = source[:, (h // 2) * LANES:(h // 2 + 1) * LANES] * scale
            if h % 2 != group % 2:
                part = pltpu.roll(part, half, 1)
            target[h] = jnp.where((lane // half) == group % 2, part, 0.0).astype(BF16)
    loads[6].wait()
    gate_all = jax.nn.sigmoid(mm_t(tokens, wg[...]))
    gate_cols = gate_all.shape[1]
    gate_pad = jnp.concatenate([gate_all, jnp.zeros((rows, LANES - gate_cols), F32)], axis=1)
    gates[...] = pltpu.roll(gate_pad, lax.rem(LANES - my_tp * 2 * heads, LANES), 1)

    def wait_slab(d, carry):
        slab_copy(d, me).wait_recv()
        return carry

    lax.fori_loop(0, me, wait_slab, 0)
    loads[7].wait()

    slab_devs = min(n_kv, 8)
    n_slabs = n_kv // slab_devs
    stacked = heads * chunk
    sel_lane = iota((chunk, slab_devs * SEL), 1)
    sel_row = iota((chunk, slab_devs * SEL), 0)
    span_lane = iota((chunk, n_kv * SPAN_PAD), 1)
    span_row = iota((chunk, n_kv * SPAN_PAD), 0)
    span_keys = gath[:, SEL:, :LANES].reshape(n_kv * SPAN_PAD, LANES)
    span_values = gath[:, SEL:, LANES:].reshape(n_kv * SPAN_PAD, LANES)
    span_id = (span_lane // SPAN_PAD) * spans_dev + span_lane % SPAN_PAD
    chunk_lane = iota((chunk, LANES), 1)

    def masked(scores, mask):
        cube = scores.reshape(heads, chunk, scores.shape[1])
        return jnp.where(mask[None], cube, big_negative).reshape(scores.shape)

    def attend(which, slot_rows):
        start = pl.multiple_of(which * chunk, chunk)
        local_block = start // SEL
        block_start = pl.multiple_of(local_block * SEL, SEL)
        in_block = start - block_start
        gath[me, :SEL, :] = own[pl.ds(block_start, SEL), :]

        qp = qp_heads[:, pl.ds(start, chunk), :].reshape(stacked, LANES)
        qt = qt_heads[:, pl.ds(start, chunk), :].reshape(stacked, LANES)

        place = me * rows + start + span_row
        allowed = (span_lane % SPAN_PAD < spans_dev) & (span_id * CMP + CMP - 1 <= place)
        s = masked(mm_t(qp, span_keys), allowed)
        span_peak = jnp.max(s, axis=1, keepdims=True)
        w = jnp.exp(s - span_peak)
        span_sum = jnp.sum(w, axis=1, keepdims=True)
        span_out = mm(w.astype(BF16), span_values)

        def slab_step(i, carry):
            base_dev = i * slab_devs
            keys = gath[pl.ds(base_dev, slab_devs), :SEL, :LANES].reshape(slab_devs * SEL, LANES)
            vals = gath[pl.ds(base_dev, slab_devs), :SEL, LANES:].reshape(slab_devs * SEL, LANES)
            dev = base_dev + sel_lane // SEL
            member = dev == chosen_ref[local_block, 0]
            for j in range(1, n_chosen):
                member = member | (dev == chosen_ref[local_block, j])
            ok = (member & (dev < me)) | ((dev == me) & (sel_lane % SEL <= sel_row + in_block))
            sc = masked(mm_t(qt, keys), ok)
            peak = jnp.max(sc, axis=1, keepdims=True)
            if carry is None:
                e = jnp.exp(sc - peak)
                return peak, jnp.sum(e, axis=1, keepdims=True), mm(e.astype(BF16), vals)
            old_peak, old_sum, old_out = carry
            peak = jnp.maximum(peak, old_peak)
            factor = jnp.exp(old_peak - peak)
            e = jnp.exp(sc - peak) * jnp.where(sc > 0.5 * big_negative, 1.0, 0.0)
            return (
                peak,
                old_sum * factor + jnp.sum(e, axis=1, keepdims=True),
                old_out * factor + mm(e.astype(BF16), vals),
            )

        if n_slabs == 1:
            sel_peak, sel_sum, sel_out = slab_step(0, None)
        else:
            sel_peak, sel_sum, sel_out = lax.fori_loop(
                0, n_slabs, slab_step,
                (
                    jnp.full((stacked, 1), big_negative, F32),
                    jnp.zeros((stacked, 1), F32),
                    jnp.zeros((stacked, LANES), F32),
                ),
            )

        has_span = (me * rows + start + iota((chunk, 1), 0)) >= CMP - 1
        gate = gates[pl.ds(start, chunk), :]
        lse0 = jnp.zeros((chunk, LANES), F32)
        lse1 = jnp.zeros((chunk, LANES), F32)
        even = None
        for h in range(heads):
            piece = slice(h * chunk, (h + 1) * chunk)
            ssum = jnp.where(has_span, span_sum[piece], 1.0)
            g0 = jnp.where(has_span, gate[:, 2 * h:2 * h + 1] / ssum, 0.0)
            g1 = gate[:, 2 * h + 1:2 * h + 2] / sel_sum[piece]
            l0 = jnp.where(has_span, span_peak[piece] + jnp.log(ssum), 0.0)
            l1 = sel_peak[piece] + jnp.log(sel_sum[piece])
            lse0 = jnp.where(chunk_lane == h, l0, lse0)
            lse1 = jnp.where(chunk_lane == h, l1, lse1)
            both = g0 * span_out[piece] + g1 * sel_out[piece]
            if h % 2 != (h // per_group) % 2:
                both = pltpu.roll(both, half, 1)
            if h % 2 == 0:
                even = both
            else:
                pair = jnp.where(chunk_lane < half, even, both).astype(BF16)
                mixed[slot_rows:slot_rows + chunk, (h // 2) * LANES:(h // 2 + 1) * LANES] = pair
        lse_rows[0, pl.ds(start, chunk), :] = lse0
        lse_rows[1, pl.ds(start, chunk), :] = lse1

    def pair_copy(t):
        return pltpu.make_async_remote_copy(
            src_ref=pair_send.at[t], dst_ref=pair_recv.at[t],
            send_sem=pair_ss.at[t], recv_sem=pair_rs.at[t],
            device_id={"tp": my_x * 2 + 1 - my_core}, device_id_type=MESH,
        )

    def cross_copy(t):
        return pltpu.make_async_remote_copy(
            src_ref=cross_send.at[t - 1], dst_ref=cross_recv.at[t - 1],
            send_sem=cross_ss.at[t - 1], recv_sem=cross_rs.at[t - 1],
            device_id={"tp": lax.rem(my_x + t, n_x) * 2 + my_core}, device_id_type=MESH,
        )

    for t in range(n_x - 1, -1, -1):
        chip = lax.rem(my_x + t, n_x)
        attend(chip * 2 + 1 - my_core, 0)
        attend(chip * 2 + my_core, chunk)
        partial = mm(mixed[...], wo[...])
        pair_send[t] = partial[:chunk].astype(BF16)
        pair_copy(t).start()
        mine = partial[chunk:]
        pair_copy(t).wait_recv()
        mine = mine + pair_recv[t].astype(F32)
        if t > 0:
            cross_send[t - 1] = mine.astype(BF16)
            cross_copy(t).start()
        else:
            for u in range(n_x - 1, 0, -1):
                cross_copy(u).wait_recv()
                mine = mine + cross_recv[u - 1].astype(F32)
            out_ref[...] = mine.astype(BF16)
            for b in range(2):
                lse_ref[b] = jnp.transpose(lse_rows[b])[:heads]

    for t in range(n_x):
        pair_copy(t).wait_send()
        if t > 0:
            cross_copy(t).wait_send()

    def wait_sent(i, carry):
        slab_copy(me, n_kv - 1 - i).wait_send()
        return carry

    lax.fori_loop(0, n_kv - 1 - me, wait_sent, 0)


def rope_tables(rows, n_kv, head_size):
    inverse = np.power(rope_base, -np.arange(head_size // 2, dtype=np.float64) * 2.0 / head_size)
    inverse = np.tile(inverse, LANES // (head_size // 2))[None, :]
    near = np.arange(rows, dtype=np.float64)[:, None] * inverse
    far = np.arange(n_kv, dtype=np.float64)[:, None] * rows * inverse
    stack = lambda a: np.stack([np.cos(a), np.sin(a)]).astype(np.float32)
    return stack(near), stack(far)


def shards(
    n_kv, n_tp,
    tokens, query_weight, key_weight, value_weight, gate_weight,
    query_gain, key_gain, out_weight, shared_block, chosen_device,
):
    rows, width = tokens.shape
    head_size = query_gain.shape[0]
    heads = query_weight.shape[1] // head_size
    group_width = key_weight.shape[1]
    groups = group_width // head_size
    if group_width < LANES:
        pad = ((0, 0), (0, LANES - group_width))
        key_weight = jnp.pad(key_weight, pad)
        value_weight = jnp.pad(value_weight, pad)
    n_x = n_tp // 2
    chunk = rows // n_tp
    inner = heads * head_size
    d_out = out_weight.shape[1]
    near, far = rope_tables(rows, n_kv, head_size)
    hbm = pl.BlockSpec(memory_space=pl.ANY)
    vmem = pl.BlockSpec(memory_space=pltpu.VMEM)
    smem = pl.BlockSpec(memory_space=pltpu.SMEM)
    dma = pltpu.SemaphoreType.DMA
    mixed_out, lse = pl.pallas_call(
        functools.partial(layer_kernel, n_kv, n_tp, heads, groups, head_size),
        out_shape=(
            pltpu.VMEM((chunk, d_out), BF16),
            pltpu.VMEM((2, heads, rows), F32),
        ),
        in_specs=[hbm] * 8 + [vmem] * 2 + [smem] * 2,
        out_specs=(vmem, vmem),
        scratch_shapes=[
            pltpu.VMEM((rows, width), BF16),
            pltpu.VMEM((width, inner), BF16),
            pltpu.VMEM((width, 2 * LANES), BF16),
            pltpu.VMEM(gate_weight.shape[::-1], BF16),
            pltpu.VMEM((inner, d_out), BF16),
            pltpu.VMEM(near.shape, F32),
            pltpu.VMEM(far.shape, F32),
            pltpu.VMEM((rows, 2 * LANES), BF16),
            pltpu.VMEM((SEL + SPAN_PAD, 2 * LANES), BF16),
            pltpu.VMEM((n_kv, SEL + SPAN_PAD, 2 * LANES), BF16),
            pltpu.VMEM((heads, rows, LANES), BF16),
            pltpu.VMEM((heads, rows, LANES), BF16),
            pltpu.VMEM((rows, LANES), F32),
            pltpu.VMEM((2 * chunk, inner), BF16),
            pltpu.VMEM((2, rows, LANES), F32),
            pltpu.VMEM((n_x, chunk, d_out), BF16),
            pltpu.VMEM((n_x, chunk, d_out), BF16),
            pltpu.VMEM((n_x - 1, chunk, d_out), BF16),
            pltpu.VMEM((n_x - 1, chunk, d_out), BF16),
            dma((8,)),
            dma((n_kv,)),
            dma((n_kv,)),
            dma((n_x,)),
            dma((n_x,)),
            dma((n_x - 1,)),
            dma((n_x - 1,)),
        ],
        compiler_params=pltpu.CompilerParams(
            collective_id=0, has_side_effects=True, vmem_limit_bytes=60 * 1024 * 1024
        ),
        name="layer",
    )(
        tokens, query_weight, key_weight, value_weight, gate_weight.T, out_weight,
        jnp.asarray(near), jnp.asarray(far),
        query_gain.reshape(1, head_size), key_gain.reshape(1, head_size),
        shared_block, chosen_device,
    )
    return mixed_out, jnp.transpose(lse, (0, 2, 1))


def solution(mesh):
    placed = (
        P("kv", None),
        P(None, "tp"),
        P(None, "tp"),
        P(None, "tp"),
        P(),
        P(),
        P(),
        P("tp", None),
        P("kv"),
        P("kv", None),
    )
    return jax.shard_map(
        functools.partial(shards, mesh.shape["kv"], mesh.shape["tp"]),
        mesh=mesh,
        in_specs=placed,
        out_specs=(P(("kv", "tp"), None), P(None, "kv", "tp")),
        check_vma=False,
    )
```

```python
import functools

import jax
import jax.numpy as jnp
import numpy as np
from jax import lax
from jax.experimental import pallas as pl
from jax.experimental.pallas import tpu as pltpu
from jax.sharding import PartitionSpec as P

SEL = 64
CMP = 32
LANES = 128
SPAN_PAD = 16
PIECES = 2

norm_eps = 1e-06
rope_base = 500000.0
big_negative = -1e30

F32 = jnp.float32
BF16 = jnp.bfloat16
MESH = pl.DeviceIdType.MESH


def mm(a, b):
    return lax.dot_general(a, b, (((1,), (0,)), ((), ())), preferred_element_type=F32)


def mm_t(a, b):
    return lax.dot_general(a, b, (((1,), (1,)), ((), ())), preferred_element_type=F32)


def iota(shape, dim):
    return lax.broadcasted_iota(jnp.int32, shape, dim)


def tile_lanes(row, times):
    return row if times == 1 else jnp.concatenate([row] * times, axis=1)


def layer_kernel(
    n_kv, n_tp, heads, groups, head_size,
    tok_hbm, wq_hbm, wk_hbm, wv_hbm, wg_hbm, wo_hbm, tab_hbm, base_hbm,
    qgain_ref, kgain_ref, shared_ref, chosen_ref,
    out_ref, lse_ref,
    tok, wq, wkv, wg, wo, tab, base,
    own, slab, gath, qp_heads, qt_heads, gates, mixed, lse_rows,
    pair_send, pair_recv, cross_send, cross_recv,
    load_sem, slab_ss, slab_rs, pair_ss, pair_rs, cross_ss, cross_rs,
):
    rows = tok.shape[0]
    per_group = heads // groups
    half = LANES // 2
    n_x = n_tp // 2
    rows_out = rows // n_tp
    n_chosen = chosen_ref.shape[1]
    me = lax.axis_index("kv")
    my_tp = lax.axis_index("tp")
    my_x = my_tp // 2
    my_core = my_tp % 2

    loads = [
        pltpu.make_async_copy(src, dst, load_sem.at[i])
        for i, (src, dst) in enumerate([
            (tok_hbm, tok),
            (wk_hbm, wkv.at[:, 0:LANES]),
            (wv_hbm, wkv.at[:, LANES:2 * LANES]),
            (tab_hbm, tab),
            (base_hbm, base),
            (wq_hbm, wq),
            (wg_hbm, wg),
            (wo_hbm, wo),
        ])
    ]
    for copy in loads:
        copy.start()

    barrier = pltpu.get_barrier_semaphore()

    def greet_kv(d, carry):
        @pl.when(d != me)
        def _():
            pl.semaphore_signal(barrier, inc=1, device_id={"kv": d}, device_id_type=MESH)
        return carry

    lax.fori_loop(0, n_kv, greet_kv, 0)
    for t in range(1, n_tp):
        peer = lax.rem(my_tp + t, n_tp)
        pl.semaphore_signal(barrier, inc=1, device_id={"tp": peer}, device_id_type=MESH)

    def clear(d, carry):
        gath[d] = jnp.zeros(gath.shape[1:], BF16)
        return carry

    lax.fori_loop(me + 1, n_kv, clear, 0)

    big = 2 * LANES
    row_i = iota((big, big), 0)
    col_i = iota((big, big), 1)
    block_mean = jnp.where(row_i // head_size == col_i // head_size, 1.0 / head_size, 0.0).astype(BF16)
    hs2 = head_size // 2
    first = (col_i % head_size) < hs2
    swap = jnp.where(
        first & (row_i == col_i + hs2), -1.0,
        jnp.where((~first) & (row_i == col_i - hs2), 1.0, 0.0),
    ).astype(BF16)

    def by_tiles(x, mat):
        width = x.shape[1]
        step = min(width, big)
        parts = [mm(x[:, i:i + step], mat[:step, :step]) for i in range(0, width, step)]
        return parts[0] if len(parts) == 1 else jnp.concatenate(parts, axis=1)

    def unit_norm(x, gain_row):
        sq = x * x
        hi = sq.astype(BF16)
        lo = (sq - hi.astype(F32)).astype(BF16)
        mean = by_tiles(hi, block_mean) + by_tiles(lo, block_mean)
        return (x * lax.rsqrt(mean + norm_eps) * gain_row).astype(BF16)

    loads[3].wait()
    loads[4].wait()
    cos_b = base[0, pl.ds(me, 1), :]
    sin_b = base[1, pl.ds(me, 1), :]
    cos_t = tab[0] * cos_b - tab[1] * sin_b
    sin_t = tab[1] * cos_b + tab[0] * sin_b

    def rotate(x):
        times = x.shape[1] // LANES
        return x.astype(F32) * tile_lanes(cos_t, times) + by_tiles(x, swap) * tile_lanes(sin_t, times)

    loads[0].wait()
    loads[1].wait()
    loads[2].wait()
    tokens = tok[...]
    kv_raw = mm(tokens, wkv[...]).astype(BF16)
    values = kv_raw[:, LANES:]
    k_gain = tile_lanes(kgain_ref[...], LANES // head_size)
    k_plain = unit_norm(kv_raw[:, :LANES].astype(F32), k_gain)
    k_turned = rotate(k_plain).astype(BF16)
    own[:, :LANES] = k_turned
    own[:, LANES:] = values
    spans_dev = rows // CMP
    avg = jnp.where(
        iota((SPAN_PAD, rows), 1) // CMP == iota((SPAN_PAD, rows), 0), 1.0 / CMP, 0.0
    ).astype(BF16)
    summary_k = mm(avg, k_plain).astype(BF16)
    summary_v = mm(avg, values).astype(BF16)
    slab[SEL:, :LANES] = summary_k
    slab[SEL:, LANES:] = summary_v
    gath[me, SEL:, :LANES] = summary_k
    gath[me, SEL:, LANES:] = summary_v
    pick = iota((SEL, rows), 1) == iota((SEL, rows), 0) + shared_ref[0] * SEL
    pick = jnp.where(pick, 1.0, 0.0).astype(BF16)
    slab[:SEL, :LANES] = mm(pick, k_turned).astype(BF16)
    slab[:SEL, LANES:] = mm(pick, values).astype(BF16)

    pl.semaphore_wait(barrier, n_kv - 1 + n_tp - 1)

    def slab_copy(slot, dst):
        return pltpu.make_async_remote_copy(
            src_ref=slab, dst_ref=gath.at[slot],
            send_sem=slab_ss.at[dst], recv_sem=slab_rs.at[slot],
            device_id={"kv": dst}, device_id_type=MESH,
        )

    def send_slab(i, carry):
        slab_copy(me, me + 1 + i).start()
        return carry

    lax.fori_loop(0, n_kv - 1 - me, send_slab, 0)

    loads[5].wait()
    lane = iota((rows, LANES), 1)
    q_raw = mm(tokens, wq[...]).astype(BF16).astype(F32)
    q_gain = tile_lanes(qgain_ref[...], heads)
    q_plain = unit_norm(q_raw, q_gain)
    q_turned = rotate(q_plain).astype(BF16).astype(F32)
    q_plain = q_plain.astype(F32)
    scale = head_size ** (-0.5)
    for source, target in ((q_plain, qp_heads), (q_turned, qt_heads)):
        for h in range(heads):
            group = h // per_group
            part = source[:, (h // 2) * LANES:(h // 2 + 1) * LANES] * scale
            if h % 2 != group % 2:
                part = pltpu.roll(part, half, 1)
            target[h] = jnp.where((lane // half) == group % 2, part, 0.0).astype(BF16)
    loads[6].wait()
    pick_row = iota((2 * LANES, wg.shape[0]), 0)
    pick_head = pick_row % LANES
    pick_col = 2 * (my_tp * heads + pick_head) + pick_row // LANES
    pick_gate = (pick_head < heads) & (iota((2 * LANES, wg.shape[0]), 1) == pick_col)
    gate_weights = mm(jnp.where(pick_gate, 1.0, 0.0).astype(BF16), wg[...]).astype(BF16)
    gates[...] = jax.nn.sigmoid(mm_t(tokens, gate_weights))

    def wait_slab(d, carry):
        slab_copy(d, me).wait_recv()
        return carry

    lax.fori_loop(0, me, wait_slab, 0)
    loads[7].wait()

    slab_devs = min(n_kv, 8)
    n_slabs = n_kv // slab_devs
    span_keys = gath[:, SEL:, :LANES].reshape(n_kv * SPAN_PAD, LANES)
    span_values = gath[:, SEL:, LANES:].reshape(n_kv * SPAN_PAD, LANES)
    def attend(which, offset, chunk):
        stacked = heads * chunk
        sel_lane = iota((chunk, slab_devs * SEL), 1)
        sel_row = iota((chunk, slab_devs * SEL), 0)
        span_lane = iota((chunk, n_kv * SPAN_PAD), 1)
        span_row = iota((chunk, n_kv * SPAN_PAD), 0)
        span_id = (span_lane // SPAN_PAD) * spans_dev + span_lane % SPAN_PAD
        chunk_lane = iota((chunk, LANES), 1)

        def masked(scores, mask):
            cube = scores.reshape(heads, chunk, scores.shape[1])
            return jnp.where(mask[None], cube, big_negative).reshape(scores.shape)

        start = pl.multiple_of(which * rows_out + offset, chunk)
        local_block = start // SEL
        block_start = pl.multiple_of(local_block * SEL, SEL)
        in_block = start - block_start
        gath[me, :SEL, :] = own[pl.ds(block_start, SEL), :]

        qp = qp_heads[:, pl.ds(start, chunk), :].reshape(stacked, LANES)
        qt = qt_heads[:, pl.ds(start, chunk), :].reshape(stacked, LANES)

        place = me * rows + start + span_row
        allowed = (span_lane % SPAN_PAD < spans_dev) & (span_id * CMP + CMP - 1 <= place)
        s = masked(mm_t(qp, span_keys), allowed)
        span_peak = jnp.max(s, axis=1, keepdims=True)
        w = jnp.exp(s - span_peak)
        span_sum = jnp.sum(w, axis=1, keepdims=True)
        span_out = mm(w.astype(BF16), span_values)

        def slab_step(i, carry):
            base_dev = i * slab_devs
            keys = gath[pl.ds(base_dev, slab_devs), :SEL, :LANES].reshape(slab_devs * SEL, LANES)
            vals = gath[pl.ds(base_dev, slab_devs), :SEL, LANES:].reshape(slab_devs * SEL, LANES)
            dev = base_dev + sel_lane // SEL
            member = dev == chosen_ref[local_block, 0]
            for j in range(1, n_chosen):
                member = member | (dev == chosen_ref[local_block, j])
            ok = (member & (dev < me)) | ((dev == me) & (sel_lane % SEL <= sel_row + in_block))
            sc = masked(mm_t(qt, keys), ok)
            peak = jnp.max(sc, axis=1, keepdims=True)
            if carry is None:
                e = jnp.exp(sc - peak)
                return peak, jnp.sum(e, axis=1, keepdims=True), mm(e.astype(BF16), vals)
            old_peak, old_sum, old_out = carry
            peak = jnp.maximum(peak, old_peak)
            factor = jnp.exp(old_peak - peak)
            e = jnp.exp(sc - peak) * jnp.where(sc > 0.5 * big_negative, 1.0, 0.0)
            return (
                peak,
                old_sum * factor + jnp.sum(e, axis=1, keepdims=True),
                old_out * factor + mm(e.astype(BF16), vals),
            )

        if n_slabs == 1:
            sel_peak, sel_sum, sel_out = slab_step(0, None)
        else:
            sel_peak, sel_sum, sel_out = lax.fori_loop(
                0, n_slabs, slab_step,
                (
                    jnp.full((stacked, 1), big_negative, F32),
                    jnp.zeros((stacked, 1), F32),
                    jnp.zeros((stacked, LANES), F32),
                ),
            )

        def by_head(column):
            acc = jnp.zeros((chunk, LANES), F32)
            for h in range(heads):
                acc = jnp.where(chunk_lane == h, column[h * chunk:(h + 1) * chunk], acc)
            return acc

        has_span = (me * rows + start + iota((chunk, LANES), 0)) >= CMP - 1
        valid = chunk_lane < heads
        ssum = jnp.where(has_span & valid, by_head(span_sum), 1.0)
        lsum = jnp.where(valid, by_head(sel_sum), 1.0)
        gate = gates[pl.ds(start, chunk), :]
        g0 = jnp.where(has_span, gate[:, :LANES] / ssum, 0.0)
        g1 = gate[:, LANES:] / lsum
        even = None
        for h in range(heads):
            piece = slice(h * chunk, (h + 1) * chunk)
            both = g0[:, h:h + 1] * span_out[piece] + g1[:, h:h + 1] * sel_out[piece]
            if h % 2 != (h // per_group) % 2:
                both = pltpu.roll(both, half, 1)
            if h % 2 == 0:
                even = both
            else:
                pair = jnp.where(chunk_lane < half, even, both).astype(BF16)
                mixed[:chunk, (h // 2) * LANES:(h // 2 + 1) * LANES] = pair
        lse_rows[0, pl.ds(start, chunk), :] = jnp.where(has_span, by_head(span_peak) + jnp.log(ssum), 0.0)
        lse_rows[1, pl.ds(start, chunk), :] = by_head(sel_peak) + jnp.log(lsum)

    sub = rows_out // PIECES

    def pair_copy(t, p, n):
        part = pl.ds(p * sub, n)
        return pltpu.make_async_remote_copy(
            src_ref=pair_send.at[t, part], dst_ref=pair_recv.at[t, part],
            send_sem=pair_ss.at[t, p], recv_sem=pair_rs.at[t, p],
            device_id={"tp": my_x * 2 + 1 - my_core}, device_id_type=MESH,
        )

    def cross_copy(t, p):
        return pltpu.make_async_remote_copy(
            src_ref=cross_send.at[t - 1, p], dst_ref=cross_recv.at[t - 1, p],
            send_sem=cross_ss.at[t - 1, p], recv_sem=cross_rs.at[t - 1, p],
            device_id={"tp": lax.rem(my_x + t, n_x) * 2 + my_core}, device_id_type=MESH,
        )

    for t in range(n_x - 1, -1, -1):
        chip = lax.rem(my_x + t, n_x)
        pieces = PIECES if t > 0 else 1
        n = rows_out // pieces
        for p in range(pieces):
            part = slice(p * n, (p + 1) * n)
            attend(chip * 2 + 1 - my_core, p * n, n)
            pair_send[t, part] = mm(mixed[:n], wo[...]).astype(BF16)
            pair_copy(t, p, n).start()
            attend(chip * 2 + my_core, p * n, n)
            mine = mm(mixed[:n], wo[...])
            pair_copy(t, p, n).wait_recv()
            mine = mine + pair_recv[t, part].astype(F32)
            if t > 0:
                cross_send[t - 1, p] = mine.astype(BF16)
                cross_copy(t, p).start()
    for b in range(2):
        lse_ref[b] = jnp.transpose(lse_rows[b])[:heads]
    for p in range(PIECES):
        part = mine[p * sub:(p + 1) * sub]
        for u in range(n_x - 1, 0, -1):
            cross_copy(u, p).wait_recv()
            part = part + cross_recv[u - 1, p].astype(F32)
        out_ref[p * sub:(p + 1) * sub] = part.astype(BF16)

    for t in range(n_x):
        pieces = PIECES if t > 0 else 1
        for p in range(pieces):
            pair_copy(t, p, rows_out // pieces).wait_send()
            if t > 0:
                cross_copy(t, p).wait_send()

    def wait_sent(i, carry):
        slab_copy(me, n_kv - 1 - i).wait_send()
        return carry

    lax.fori_loop(0, n_kv - 1 - me, wait_sent, 0)


def rope_tables(rows, n_kv, head_size):
    inverse = np.power(rope_base, -np.arange(head_size // 2, dtype=np.float64) * 2.0 / head_size)
    inverse = np.tile(inverse, LANES // (head_size // 2))[None, :]
    near = np.arange(rows, dtype=np.float64)[:, None] * inverse
    far = np.arange(n_kv, dtype=np.float64)[:, None] * rows * inverse
    stack = lambda a: np.stack([np.cos(a), np.sin(a)]).astype(np.float32)
    return stack(near), stack(far)


def shards(
    n_kv, n_tp,
    tokens, query_weight, key_weight, value_weight, gate_weight,
    query_gain, key_gain, out_weight, shared_block, chosen_device,
):
    rows, width = tokens.shape
    head_size = query_gain.shape[0]
    heads = query_weight.shape[1] // head_size
    group_width = key_weight.shape[1]
    groups = group_width // head_size
    if group_width < LANES:
        pad = ((0, 0), (0, LANES - group_width))
        key_weight = jnp.pad(key_weight, pad)
        value_weight = jnp.pad(value_weight, pad)
    n_x = n_tp // 2
    chunk = rows // n_tp
    inner = heads * head_size
    d_out = out_weight.shape[1]
    near, far = rope_tables(rows, n_kv, head_size)
    hbm = pl.BlockSpec(memory_space=pl.ANY)
    vmem = pl.BlockSpec(memory_space=pltpu.VMEM)
    smem = pl.BlockSpec(memory_space=pltpu.SMEM)
    dma = pltpu.SemaphoreType.DMA
    mixed_out, lse = pl.pallas_call(
        functools.partial(layer_kernel, n_kv, n_tp, heads, groups, head_size),
        out_shape=(
            pltpu.VMEM((chunk, d_out), BF16),
            pltpu.VMEM((2, heads, rows), F32),
        ),
        in_specs=[hbm] * 8 + [vmem] * 2 + [smem] * 2,
        out_specs=(vmem, vmem),
        scratch_shapes=[
            pltpu.VMEM((rows, width), BF16),
            pltpu.VMEM((width, inner), BF16),
            pltpu.VMEM((width, 2 * LANES), BF16),
            pltpu.VMEM(gate_weight.shape[::-1], BF16),
            pltpu.VMEM((inner, d_out), BF16),
            pltpu.VMEM(near.shape, F32),
            pltpu.VMEM(far.shape, F32),
            pltpu.VMEM((rows, 2 * LANES), BF16),
            pltpu.VMEM((SEL + SPAN_PAD, 2 * LANES), BF16),
            pltpu.VMEM((n_kv, SEL + SPAN_PAD, 2 * LANES), BF16),
            pltpu.VMEM((heads, rows, LANES), BF16),
            pltpu.VMEM((heads, rows, LANES), BF16),
            pltpu.VMEM((rows, 2 * LANES), F32),
            pltpu.VMEM((chunk, inner), BF16),
            pltpu.VMEM((2, rows, LANES), F32),
            pltpu.VMEM((n_x, chunk, d_out), BF16),
            pltpu.VMEM((n_x, chunk, d_out), BF16),
            pltpu.VMEM((n_x - 1, PIECES, chunk // PIECES, d_out), BF16),
            pltpu.VMEM((n_x - 1, PIECES, chunk // PIECES, d_out), BF16),
            dma((8,)),
            dma((n_kv,)),
            dma((n_kv,)),
            dma((n_x, PIECES)),
            dma((n_x, PIECES)),
            dma((n_x - 1, PIECES)),
            dma((n_x - 1, PIECES)),
        ],
        compiler_params=pltpu.CompilerParams(
            collective_id=0, has_side_effects=True, vmem_limit_bytes=60 * 1024 * 1024
        ),
        name="layer",
    )(
        tokens, query_weight, key_weight, value_weight, gate_weight.T, out_weight,
        jnp.asarray(near), jnp.asarray(far),
        query_gain.reshape(1, head_size), key_gain.reshape(1, head_size),
        shared_block, chosen_device,
    )
    return mixed_out, jnp.transpose(lse, (0, 2, 1))


def solution(mesh):
    placed = (
        P("kv", None),
        P(None, "tp"),
        P(None, "tp"),
        P(None, "tp"),
        P(),
        P(),
        P(),
        P("tp", None),
        P("kv"),
        P("kv", None),
    )
    return jax.shard_map(
        functools.partial(shards, mesh.shape["kv"], mesh.shape["tp"]),
        mesh=mesh,
        in_specs=placed,
        out_specs=(P(("kv", "tp"), None), P(None, "kv", "tp")),
        check_vma=False,
    )
```
